1024 devices in a mesh: sp: 16 (over z), dp: 64 (over y, x, core).
Axes of the slice: x: 4, y: 8, z: 16, core: 2. Of those that a mesh axis runs over, the one named last changes fastest.
Arguments:
- queries: bfloat16 [64, 2048, 1024], P('dp', 'sp'), may hold values from -6 to 6
- key_rows: bfloat16 [64, 2048, 1024], P('dp', 'sp'), may hold values from -6 to 6
- values: bfloat16 [64, 2048, 2048], P('dp', 'sp'), may hold values from -6 to 6
- out_gate: bfloat16 [64, 2048, 2048], P('dp', 'sp'), may hold values from -6 to 6
- input_gate: bfloat16 [64, 4, 2048], P('dp', None, 'sp'), may hold values from -6 to 205
- forget_gate: bfloat16 [64, 4, 2048], P('dp', None, 'sp'), may hold values from 0.5 to 13
- out_weight: bfloat16 [2048, 2048], P(None, 'dp'), may hold values from -0.125 to 0.125
Outputs:
- layer_out: bfloat16 [64, 2048, 2048], P('dp', 'sp')
The draws below stay inside these ranges and needn't reach their ends.
All inputs are finite; a program needn't handle non-finite values.
Results may differ from the reference program's by a relative error of at most 0.0057.
Values may be sent and summed in bfloat16 or wider, within the bound.
A program may use at most 64 MiB of HBM per device.

```python
import jax
import jax.numpy as jnp
from jax import lax

D = 2048
MEMORY_UNITS = 4
DK = 256
DV = 512
BLOCK = 128
TOK_DEV = 128
STEP_TOTAL = 2048
STREAM_TOTAL = 64
VW = 2048


def draw_input_gate(key, part):
    dims_all = (STREAM_TOTAL, MEMORY_UNITS, STEP_TOTAL)
    result = jnp.clip(1.5 * jax.random.normal(jax.random.fold_in(key, 4), dims_all, jnp.float32), -6.0, 6.0)
    return result.astype(jnp.bfloat16)


def draw_forget_gate(key, part):
    dims_all = (STREAM_TOTAL, MEMORY_UNITS, STEP_TOTAL)
    multiplier = jnp.exp(jax.random.uniform(jax.random.fold_in(key, 11), (STREAM_TOTAL, MEMORY_UNITS, STEP_TOTAL // TOK_DEV, 1), jnp.float32, -0.7, 0.7))
    multiplier = jnp.broadcast_to(multiplier, (STREAM_TOTAL, MEMORY_UNITS, STEP_TOTAL // TOK_DEV, TOK_DEV)).reshape(dims_all)
    gaussian_jitter = jnp.exp(0.5 * jnp.clip(jax.random.normal(jax.random.fold_in(key, 12), dims_all, jnp.float32), -3.0, 3.0))
    ranking = jax.random.randint(jax.random.fold_in(key, 13), (STREAM_TOTAL, MEMORY_UNITS), 0, 1 << 20) * MEMORY_UNITS + lax.broadcasted_iota(jnp.int32, (STREAM_TOTAL, MEMORY_UNITS), 1)
    order = jnp.argsort(ranking, axis=1)
    position_rank = jnp.argsort(order, axis=1)
    quick_head = (position_rank < MEMORY_UNITS // 2)[:, :, None]
    background_level = jnp.where(quick_head, 1.0 / 40.0, 0.5 / STEP_TOTAL) * jnp.ones(dims_all, jnp.float32)
    spike_offset = jax.random.randint(jax.random.fold_in(key, 14), (STREAM_TOTAL, MEMORY_UNITS, 3, 1), 0, STEP_TOTAL)
    spike_indices = lax.broadcasted_iota(jnp.int32, (1, 1, 1, STEP_TOTAL), 3)
    spike_count = jnp.any(spike_indices == spike_offset, axis=2)
    spike_magnitude = jnp.where(spike_count, 0.4, background_level * multiplier * gaussian_jitter)
    gate_logits = -jnp.log(jnp.expm1(spike_magnitude))
    return gate_logits.astype(jnp.bfloat16)


def levels(rng, shape, cuts, smallest, high):
    def one(position, shards_of):
        steps = jax.random.uniform(jax.random.fold_in(jax.random.fold_in(rng, 6), position), (shards_of,), jnp.float32, smallest / len(cuts), high / len(cuts))
        return jnp.repeat(jnp.exp(steps), shape[position] // shards_of).reshape((-1,) + (1,) * (len(shape) - position - 1))

    gain = one(*cuts[0])
    for cut in cuts[1:]:
        gain = gain * one(*cut)
    return gain


def bell_draw(own_key, dims, width, bound, shards=(), dtype=jnp.bfloat16):
    entries = jax.random.normal(own_key, dims, jnp.float32) * width
    if len(shards) > 0:
        entries = levels(own_key, dims, shards, -0.22, 0.18) * entries
    return jnp.clip(entries, min=-bound, max=bound).astype(dtype)


def setup_inputs(seed: int = 0) -> dict:
    key_of = jax.random.split(jax.random.key(seed), 8)
    return {
        "queries": bell_draw(key_of[0], (STREAM_TOTAL, STEP_TOTAL, MEMORY_UNITS * DK), 1.0, 6.0, ((0, 64), (1, 16))),
        "key_rows": bell_draw(key_of[1], (STREAM_TOTAL, STEP_TOTAL, MEMORY_UNITS * DK), 1.0, 6.0, ((0, 64), (1, 16))),
        "values": bell_draw(key_of[2], (STREAM_TOTAL, STEP_TOTAL, VW), 1.0, 6.0, ((0, 64), (1, 16))),
        "out_gate": bell_draw(key_of[3], (STREAM_TOTAL, STEP_TOTAL, VW), 1.0, 6.0, ((0, 64), (1, 16))),
        "input_gate": draw_input_gate(jax.random.fold_in(key_of[7], 71), 0),
        "forget_gate": draw_forget_gate(jax.random.fold_in(key_of[7], 71), 0),
        "out_weight": bell_draw(key_of[6], (VW, D), VW ** -0.5, 0.125, ((1, 64),)),
    }


def memory_cell(query_rows, key_in, value_rows, input_log, forget_log):
    block_count = query_rows.shape[0] // BLOCK
    key_width = query_rows.shape[1]
    value_width = value_rows.shape[1]
    key_scale = key_width ** -0.5
    causal = lax.broadcasted_iota(jnp.int32, (BLOCK, BLOCK), 0) >= lax.broadcasted_iota(jnp.int32, (BLOCK, BLOCK), 1)
    highest = lax.Precision.HIGHEST

    def block_step(state_in, inputs):
        memory, normer, stabil = state_in
        query_part, key_part, value_part, gain_part, decay_part = inputs
        query_part = query_part.astype(jnp.float32)
        key_part = key_part.astype(jnp.float32) * key_scale
        value_part = value_part.astype(jnp.float32)
        running = jnp.cumsum(decay_part)
        log_weight = running[:, None] - running[None, :] + gain_part[None, :]
        log_weight = jnp.where(causal, log_weight, -jnp.inf)
        carried_log = running + stabil
        row_top = jnp.maximum(carried_log, jnp.max(log_weight, axis=1))
        scores = jnp.dot(query_part, key_part.T, precision=highest) * jnp.exp(log_weight - row_top[:, None])
        carried = jnp.exp(carried_log - row_top)
        numerator = jnp.dot(scores, value_part, precision=highest) + carried[:, None] * jnp.dot(query_part, memory, precision=highest)
        denominator = jnp.sum(scores, axis=1) + carried * jnp.dot(query_part, normer, precision=highest)
        output = numerator / jnp.maximum(jnp.abs(denominator), 1.0)[:, None]
        block_end = running[-1]
        weight_log = block_end - running + gain_part
        new_top = jnp.maximum(block_end + stabil, jnp.max(weight_log))
        weights = jnp.exp(weight_log - new_top)
        retain = jnp.exp(block_end + stabil - new_top)
        memory = retain * memory + jnp.dot((key_part * weights[:, None]).T, value_part, precision=highest)
        normer = retain * normer + jnp.dot(weights, key_part, precision=highest)
        return (memory, normer, new_top), output

    start_state = (jnp.zeros((key_width, value_width), jnp.float32), jnp.zeros((key_width,), jnp.float32), jnp.zeros((), jnp.float32))
    blocks = tuple(source.reshape((block_count, BLOCK) + source.shape[1:]) for source in (query_rows, key_in, value_rows, input_log, forget_log))
    _, outputs = lax.scan(block_step, start_state, blocks)
    return outputs.reshape(block_count * BLOCK, value_width)


def reference(queries, key_rows, values, out_gate, input_gate, forget_gate, out_weight):
    query_heads = queries.reshape(STREAM_TOTAL, STEP_TOTAL, MEMORY_UNITS, DK).transpose(0, 2, 1, 3)
    key_heads = key_rows.reshape(STREAM_TOTAL, STEP_TOTAL, MEMORY_UNITS, DK).transpose(0, 2, 1, 3)
    value_heads = values.reshape(STREAM_TOTAL, STEP_TOTAL, MEMORY_UNITS, DV).transpose(0, 2, 1, 3)
    input_log = input_gate.astype(jnp.float32)
    forget_log = jax.nn.log_sigmoid(forget_gate.astype(jnp.float32))
    per_head = jax.vmap(jax.vmap(memory_cell))
    cell_out = per_head(query_heads, key_heads, value_heads, input_log, forget_log)
    hidden = cell_out.transpose(0, 2, 1, 3).reshape(STREAM_TOTAL, STEP_TOTAL, VW).astype(jnp.bfloat16)
    hidden = lax.optimization_barrier(hidden)
    gated = (hidden.astype(jnp.float32) * jax.nn.sigmoid(out_gate.astype(jnp.float32))).astype(jnp.bfloat16)
    projected = jnp.dot(gated.reshape(STREAM_TOTAL * STEP_TOTAL, VW), out_weight, preferred_element_type=jnp.float32)
    return projected.reshape(STREAM_TOTAL, STEP_TOTAL, D).astype(jnp.bfloat16)
```

```python
import functools

import jax
import jax.numpy as jnp
from jax import lax
from jax.experimental import pallas as pl
from jax.experimental.pallas import tpu as pltpu
from jax.sharding import PartitionSpec as P

MESH = pl.DeviceIdType.MESH
HEADS = 4
DK = 256
DV = 512
T = 128
ROWS = 16
PIECES = DK // ROWS
F32 = jnp.float32
BF16 = jnp.bfloat16


def local_terms(h, q_ref, k_ref, v_ref, run, gain, part, norm_loc, top_loc, cm_scr, kcol_scr):
    row = lax.broadcasted_iota(jnp.int32, (T, T), 0)
    col = lax.broadcasted_iota(jnp.int32, (T, T), 1)
    d = gain[h : h + 1, :] - run[h : h + 1, :]
    dd = jnp.broadcast_to(d, (T, T))
    running_top = jnp.max(jnp.where(col <= row, dd, -jnp.inf), axis=1, keepdims=True)
    d_col = jnp.sum(jnp.where(col == row, dd, 0.0), axis=1, keepdims=True)
    top = jnp.max(d, axis=1, keepdims=True)
    cm_scr[h] = jnp.broadcast_to(running_top, (T, T))
    top_loc[h : h + 1, :] = jnp.broadcast_to(top, (1, DK))
    keys = k_ref[:, h * DK : (h + 1) * DK].astype(F32) * (DK**-0.5)
    weighted = keys * jnp.exp(d_col - top)
    norm_loc[h : h + 1, :] = jnp.sum(weighted, axis=0, keepdims=True)
    state = lax.dot_general(
        weighted.astype(BF16),
        v_ref[:, h * DV : (h + 1) * DV],
        (((0,), (0,)), ((), ())),
        preferred_element_type=F32,
    )
    part[h * PIECES : (h + 1) * PIECES] = state.reshape(PIECES, ROWS, DV)


def within_block(h, q_ref, k_ref, v_ref, run, gain, cm_scr, sv_scr, den_scr):
    row = lax.broadcasted_iota(jnp.int32, (T, T), 0)
    col = lax.broadcasted_iota(jnp.int32, (T, T), 1)
    d = gain[h : h + 1, :] - run[h : h + 1, :]
    weight = jnp.where(col <= row, jnp.exp(jnp.minimum(d - cm_scr[h], 0.0)), 0.0)
    raw = lax.dot_general(
        q_ref[:, h * DK : (h + 1) * DK],
        k_ref[:, h * DK : (h + 1) * DK],
        (((1,), (1,)), ((), ())),
        preferred_element_type=F32,
    )
    scores = raw * (DK**-0.5) * weight
    den_scr[h] = jnp.broadcast_to(jnp.sum(scores, axis=1, keepdims=True), (T, T))
    high = scores.astype(BF16)
    low = (scores - high.astype(F32)).astype(BF16)
    values = v_ref[:, h * DV : (h + 1) * DV]
    sv_scr[h] = jnp.dot(high, values, preferred_element_type=F32) + jnp.dot(
        low, values, preferred_element_type=F32
    )


def cell_kernel(
    q_ref,
    k_ref,
    v_ref,
    og_ref,
    ig_ref,
    fg_ref,
    out_ref,
    part,
    recv,
    send,
    head_in,
    head_out,
    norm_loc,
    top_loc,
    end_loc,
    keep_scr,
    add_scr,
    cm_scr,
    den_scr,
    sv_scr,
    gate_scr,
    send_sem,
    recv_sem,
):
    me = lax.axis_index("sp")
    size = lax.axis_size("sp")
    right = lax.rem(me + 1, size)
    left = lax.rem(me + size - 1, size)

    barrier = pltpu.get_barrier_semaphore()
    for other in (left, right):
        pl.semaphore_signal(barrier, inc=1, device_id={"sp": other}, device_id_type=MESH)

    def piece_copy(i):
        return pltpu.make_async_remote_copy(
            src_ref=send.at[i],
            dst_ref=recv.at[i],
            send_sem=send_sem.at[i],
            recv_sem=recv_sem.at[i],
            device_id={"sp": right},
            device_id_type=MESH,
        )

    last = HEADS * PIECES
    head_copy = pltpu.make_async_remote_copy(
        src_ref=head_out,
        dst_ref=head_in,
        send_sem=send_sem.at[last],
        recv_sem=recv_sem.at[last],
        device_id={"sp": right},
        device_id_type=MESH,
    )

    gain = ig_ref[...].astype(F32)
    decay = -jnp.log1p(jnp.exp(-fg_ref[...].astype(F32)))
    row = lax.broadcasted_iota(jnp.int32, (T, T), 0)
    col = lax.broadcasted_iota(jnp.int32, (T, T), 1)
    upto = jnp.where(row <= col, 1.0, 0.0).astype(F32)
    run = jnp.dot(decay, upto, precision=lax.Precision.HIGHEST, preferred_element_type=F32)
    end_loc[...] = jnp.broadcast_to(run[:, T - 1 : T], (HEADS, DK))
    for h in range(HEADS):
        local_terms(h, q_ref, k_ref, v_ref, run, gain, part, norm_loc, top_loc, cm_scr, None)

    pl.semaphore_wait(barrier, 2)

    def step_header(stab, norm):
        new = jnp.maximum(stab, top_loc[...])
        keep = jnp.exp(stab - new)
        add = jnp.exp(top_loc[...] - new)
        head_out[0:HEADS, :] = end_loc[...] + new
        head_out[HEADS:, :] = keep * norm + add * norm_loc[...]
        keep_scr[...] = jnp.concatenate([keep, keep], axis=1)
        add_scr[...] = jnp.concatenate([add, add], axis=1)

    @pl.when(me == 0)
    def _():
        head_in[...] = jnp.zeros((2 * HEADS, DK), F32)
        step_header(jnp.zeros((HEADS, DK), F32), jnp.zeros((HEADS, DK), F32))
        head_copy.start()
        for h in range(HEADS):

            def first(i, _, h=h):
                at = h * PIECES + i
                send[at] = (add_scr[h : h + 1, :] * part[at]).astype(BF16)
                piece_copy(at).start()
                return 0

            lax.fori_loop(0, PIECES, first, 0)

        def clear(i, _):
            recv[i] = jnp.zeros((ROWS, DV), BF16)
            return 0

        lax.fori_loop(0, last, clear, 0)

    for h in range(HEADS):
        within_block(h, q_ref, k_ref, v_ref, run, gain, cm_scr, sv_scr, den_scr)
        gate_scr[:, h * DV : (h + 1) * DV] = jax.nn.sigmoid(
            og_ref[:, h * DV : (h + 1) * DV].astype(F32)
        )

    def consume(h):
        q = q_ref[:, h * DK : (h + 1) * DK]
        stab = head_in[h : h + 1, 0:T]
        norm = head_in[HEADS + h : HEADS + h + 1, :]
        top = jnp.maximum(stab, cm_scr[h])
        own = jnp.exp(cm_scr[h] - top)
        old = jnp.exp(stab - top)
        past = jnp.sum(q.astype(F32) * norm, axis=1, keepdims=True)
        den = own * den_scr[h] + old * past
        inv = 1.0 / jnp.maximum(jnp.abs(den), 1.0)
        own = own * inv
        old = old * inv
        state = recv[h * PIECES : (h + 1) * PIECES].reshape(DK, DV)
        carried = jnp.dot(q, state, preferred_element_type=F32)
        for c in range(DV // T):
            at = slice(c * T, (c + 1) * T)
            cell = own * sv_scr[h, :, at] + old * carried[:, at]
            hidden = cell.astype(BF16).astype(F32)
            cols = slice(h * DV + c * T, h * DV + (c + 1) * T)
            out_ref[:, cols] = (hidden * gate_scr[:, cols]).astype(BF16)

    @pl.when(jnp.logical_and(me > 0, me < size - 1))
    def _():
        head_copy.wait_recv()
        step_header(head_in[0:HEADS, :], head_in[HEADS:, :])
        head_copy.start()
        for h in range(HEADS):

            def middle(i, _, h=h):
                at = h * PIECES + i
                piece_copy(at).wait_recv()
                new = keep_scr[h : h + 1, :] * recv[at].astype(F32) + add_scr[h : h + 1, :] * part[at]
                send[at] = new.astype(BF16)
                piece_copy(at).start()
                return 0

            lax.fori_loop(0, PIECES, middle, 0)

    @pl.when(me == size - 1)
    def _():
        head_copy.wait_recv()

    for h in range(HEADS):

        @pl.when(me == size - 1)
        def _(h=h):
            def final(i, _):
                piece_copy(h * PIECES + i).wait_recv()
                return 0

            lax.fori_loop(0, PIECES, final, 0)

        consume(h)

    @pl.when(me < size - 1)
    def _():
        head_copy.wait_send()

        def drain(i, _):
            piece_copy(i).wait_send()
            return 0

        lax.fori_loop(0, last, drain, 0)


def cell(q, k, v, og, ig, fg):
    pieces = HEADS * PIECES
    return pl.pallas_call(
        cell_kernel,
        out_shape=jax.ShapeDtypeStruct((T, HEADS * DV), BF16),
        in_specs=[pl.BlockSpec(memory_space=pltpu.VMEM)] * 6,
        out_specs=pl.BlockSpec(memory_space=pltpu.VMEM),
        scratch_shapes=[
            pltpu.VMEM((pieces, ROWS, DV), F32),
            pltpu.VMEM((pieces, ROWS, DV), BF16),
            pltpu.VMEM((pieces, ROWS, DV), BF16),
            pltpu.VMEM((2 * HEADS, DK), F32),
            pltpu.VMEM((2 * HEADS, DK), F32),
            pltpu.VMEM((HEADS, DK), F32),
            pltpu.VMEM((HEADS, DK), F32),
            pltpu.VMEM((HEADS, DK), F32),
            pltpu.VMEM((HEADS, DV), F32),
            pltpu.VMEM((HEADS, DV), F32),
            pltpu.VMEM((HEADS, T, T), F32),
            pltpu.VMEM((HEADS, T, T), F32),
            pltpu.VMEM((HEADS, T, DV), F32),
            pltpu.VMEM((T, HEADS * DV), F32),
            pltpu.SemaphoreType.DMA((pieces + 1,)),
            pltpu.SemaphoreType.DMA((pieces + 1,)),
        ],
        compiler_params=pltpu.CompilerParams(collective_id=0, has_side_effects=True),
        cost_estimate=pl.CostEstimate(flops=10**11, bytes_accessed=2 * 10**7, transcendentals=0),
    )(q, k, v, og, ig, fg)


def body(queries, key_rows, values, out_gate, input_gate, forget_gate, out_weight):
    whole_weight = lax.all_gather(out_weight, "dp", axis=1, tiled=True)
    gated = cell(
        queries[0], key_rows[0], values[0], out_gate[0], input_gate[0], forget_gate[0]
    )
    projected = jnp.dot(gated, whole_weight, preferred_element_type=F32)
    return projected.astype(BF16)[None]


def solution(mesh):
    return jax.shard_map(
        body,
        mesh=mesh,
        in_specs=(
            P("dp", "sp", None),
            P("dp", "sp", None),
            P("dp", "sp", None),
            P("dp", "sp", None),
            P("dp", None, "sp"),
            P("dp", None, "sp"),
            P(None, "dp"),
        ),
        out_specs=P("dp", "sp", None),
        check_vma=False,
    )
```

```python
import functools

import jax
import jax.numpy as jnp
from jax import lax
from jax.experimental import pallas as pl
from jax.experimental.pallas import tpu as pltpu
from jax.sharding import PartitionSpec as P

MESH = pl.DeviceIdType.MESH
HEADS = 4
DK = 256
DV = 512
T = 128
ROWS = 16
PIECES = DK // ROWS
NX = 4
NY = 8
HALF = 16
START = (1, 3, 6, 8, 10, 10)
F32 = jnp.float32
BF16 = jnp.bfloat16


def local_terms(h, q_ref, k_ref, v_ref, run, gain, part, norm_loc, top_loc, cm_scr, kcol_scr):
    row = lax.broadcasted_iota(jnp.int32, (T, T), 0)
    col = lax.broadcasted_iota(jnp.int32, (T, T), 1)
    d = gain[h : h + 1, :] - run[h : h + 1, :]
    dd = jnp.broadcast_to(d, (T, T))
    running_top = jnp.max(jnp.where(col <= row, dd, -jnp.inf), axis=1, keepdims=True)
    d_col = jnp.sum(jnp.where(col == row, dd, 0.0), axis=1, keepdims=True)
    top = jnp.max(d, axis=1, keepdims=True)
    cm_scr[h] = jnp.broadcast_to(running_top, (T, T))
    top_loc[h : h + 1, :] = jnp.broadcast_to(top, (1, DK))
    keys = k_ref[:, h * DK : (h + 1) * DK].astype(F32) * (DK**-0.5)
    weighted = keys * jnp.exp(d_col - top)
    norm_loc[h : h + 1, :] = jnp.sum(weighted, axis=0, keepdims=True)
    state = lax.dot_general(
        weighted.astype(BF16),
        v_ref[:, h * DV : (h + 1) * DV],
        (((0,), (0,)), ((), ())),
        preferred_element_type=F32,
    )
    part[h * PIECES : (h + 1) * PIECES] = state.reshape(PIECES, ROWS, DV)


def within_block(h, q_ref, k_ref, v_ref, run, gain, cm_scr, sv_scr, den_scr):
    row = lax.broadcasted_iota(jnp.int32, (T, T), 0)
    col = lax.broadcasted_iota(jnp.int32, (T, T), 1)
    d = gain[h : h + 1, :] - run[h : h + 1, :]
    weight = jnp.where(col <= row, jnp.exp(jnp.minimum(d - cm_scr[h], 0.0)), 0.0)
    raw = lax.dot_general(
        q_ref[:, h * DK : (h + 1) * DK],
        k_ref[:, h * DK : (h + 1) * DK],
        (((1,), (1,)), ((), ())),
        preferred_element_type=F32,
    )
    scores = raw * (DK**-0.5) * weight
    den_scr[h] = jnp.broadcast_to(jnp.sum(scores, axis=1, keepdims=True), (T, T))
    high = scores.astype(BF16)
    low = (scores - high.astype(F32)).astype(BF16)
    values = v_ref[:, h * DV : (h + 1) * DV]
    sv_scr[h] = jnp.dot(high, values, preferred_element_type=F32) + jnp.dot(
        low, values, preferred_element_type=F32
    )


def cell_kernel(
    q_ref,
    k_ref,
    v_ref,
    og_ref,
    ig_ref,
    fg_ref,
    w_ref,
    out_ref,
    part,
    recv,
    send,
    head_in,
    head_out,
    norm_loc,
    top_loc,
    end_loc,
    keep_scr,
    add_scr,
    cm_scr,
    den_scr,
    sv_scr,
    gate_scr,
    gated,
    acc,
    wa,
    wb,
    send_sem,
    recv_sem,
    wa_recv,
    wb_recv,
    w_send,
    pair_send,
    pair_recv,
):
    me = lax.axis_index("sp")
    size = lax.axis_size("sp")
    right = lax.rem(me + 1, size)
    left = lax.rem(me + size - 1, size)

    place = lax.axis_index("dp")
    core = lax.rem(place, 2)
    x = lax.rem(lax.div(place, 2), NX)
    y = lax.div(place, 2 * NX)

    def wrap(a, n):
        return lax.rem(a + n, n)

    def device(xx, yy, cc):
        return yy * (2 * NX) + xx * 2 + cc

    x_up = device(wrap(x + 1, NX), y, core)
    x_down = device(wrap(x - 1, NX), y, core)
    y_up = device(x, wrap(y + 1, NY), core)
    y_down = device(x, wrap(y - 1, NY), core)
    pair = device(x, y, 1 - core)

    barrier = pltpu.get_barrier_semaphore()
    for other in (left, right):
        pl.semaphore_signal(barrier, inc=1, device_id={"sp": other}, device_id_type=MESH)
    for other in (x_up, x_down, y_up, y_down, pair):
        pl.semaphore_signal(barrier, inc=1, device_id={"dp": other}, device_id_type=MESH)

    kinds = ((wa, wa_recv, 0), (wb, wb_recv, 1))

    def slot(kind, xx, yy):
        return yy * NX + xx if kind == 0 else xx * NY + yy

    def block_send(kind, xx, yy, to, own=False):
        buf, arrived, which = kinds[kind]
        at = slot(kind, xx, yy)
        src = w_ref.at[pl.ds(kind * HALF, HALF)] if own else buf.at[core, at]
        pltpu.make_async_remote_copy(
            src_ref=src,
            dst_ref=buf.at[core, at],
            send_sem=w_send.at[which],
            recv_sem=arrived.at[at],
            device_id={"dp": to},
            device_id_type=MESH,
        ).start()

    def pair_copy(kind, xx, yy, own=False):
        buf, _, which = kinds[kind]
        at = slot(kind, xx, yy)
        src = w_ref.at[pl.ds(kind * HALF, HALF)] if own else buf.at[core, at]
        pltpu.make_async_remote_copy(
            src_ref=src,
            dst_ref=buf.at[core, at],
            send_sem=pair_send.at[which],
            recv_sem=pair_recv.at[which],
            device_id={"dp": pair},
            device_id_type=MESH,
        ).start()

    def block_wait(kind, xx, yy):
        buf, arrived, which = kinds[kind]
        at = slot(kind, xx, yy)
        pltpu.make_async_remote_copy(
            src_ref=buf.at[core, at],
            dst_ref=buf.at[core, at],
            send_sem=w_send.at[which],
            recv_sem=arrived.at[at],
            device_id={"dp": pair},
            device_id_type=MESH,
        ).wait_recv()

    turn = 1 - 2 * core

    def gather_own():
        for kind in range(2):
            for to in (x_up, x_down, y_up, y_down) if kind == 0 else (y_up, y_down, x_up, x_down):
                block_send(kind, x, y, to, own=True)
            pair_copy(kind, x, y, own=True)

    def first_event(o, t):
        xx, yy = wrap(x + o, NX), wrap(y - t, NY)
        block_wait(0, xx, yy)
        if t == 0 or t in (1, 2) or (t == 3 and o in (0, 1)):
            block_send(0, xx, yy, y_up)
        if t == 0 or t in (-1, -2) or (t == -3 and o in (-1, 2)):
            block_send(0, xx, yy, y_down)
        pair_copy(0, xx, yy)

    def second_event(o, t):
        xx, yy = wrap(x - o, NX), wrap(y - t, NY)
        block_wait(1, xx, yy)
        if o == 0 and t in (1, 2):
            block_send(1, xx, yy, y_up)
        if o == 0 and t in (-1, -2):
            block_send(1, xx, yy, y_down)
        if o == 0 or (o == 1 and t in (0, 1, 2, 3)):
            block_send(1, xx, yy, x_up)
        if o == 0 or (o == -1 and t not in (0, 1, 2, 3)):
            block_send(1, xx, yy, x_down)
        pair_copy(1, xx, yy)

    def gather_round(hops):
        for t in (0, 1, -1, 2, -2, 3, -3, 4):
            for o in (0, 1, -1, 2):
                if abs(o) + abs(t) == hops:
                    first_event(o, t)
                    if (o, t) == (-1, 0):
                        block_send(
                            0, wrap(x - turn, NX), y, device(wrap(x + turn, NX), y, core)
                        )
        for o in (0, 1, -1, 2):
            for t in (0, 1, -1, 2, -2, 3, -3, 4):
                if abs(o) + abs(t) == hops:
                    second_event(o, t)
                    if (o, t) == (0, -3):
                        block_send(
                            1, x, wrap(y - 3 * turn, NY), device(x, wrap(y + turn, NY), core)
                        )

    def gather_end():
        for buf, _, which in kinds:
            whole = pltpu.make_async_remote_copy(
                src_ref=buf.at[core],
                dst_ref=buf.at[1 - core],
                send_sem=pair_send.at[which],
                recv_sem=pair_recv.at[which],
                device_id={"dp": pair},
                device_id_type=MESH,
            )
            whole.wait_recv()
            whole.wait_send()
            sent = buf.at[core, pl.ds(0, NX * NY - 1)]
            pltpu.make_async_remote_copy(
                src_ref=sent,
                dst_ref=sent,
                send_sem=w_send.at[which],
                recv_sem=pair_recv.at[which],
                device_id={"dp": pair},
                device_id_type=MESH,
            ).wait_send()

    def piece_copy(i):
        return pltpu.make_async_remote_copy(
            src_ref=send.at[i],
            dst_ref=recv.at[i],
            send_sem=send_sem.at[0],
            recv_sem=recv_sem.at[i],
            device_id={"sp": right},
            device_id_type=MESH,
        )

    last = HEADS * PIECES
    head_copy = pltpu.make_async_remote_copy(
        src_ref=head_out,
        dst_ref=head_in,
        send_sem=send_sem.at[1],
        recv_sem=recv_sem.at[last],
        device_id={"sp": right},
        device_id_type=MESH,
    )

    gain = ig_ref[...].astype(F32)
    decay = -jnp.log1p(jnp.exp(-fg_ref[...].astype(F32)))
    row = lax.broadcasted_iota(jnp.int32, (T, T), 0)
    col = lax.broadcasted_iota(jnp.int32, (T, T), 1)
    upto = jnp.where(row <= col, 1.0, 0.0).astype(F32)
    run = jnp.dot(decay, upto, precision=lax.Precision.HIGHEST, preferred_element_type=F32)
    end_loc[...] = jnp.broadcast_to(run[:, T - 1 : T], (HEADS, DK))
    for h in range(HEADS):
        local_terms(h, q_ref, k_ref, v_ref, run, gain, part, norm_loc, top_loc, cm_scr, None)

    pl.semaphore_wait(barrier, 7)
    @pl.when(me > 0)
    def _():
        gather_own()

    wa[core, slot(0, x, y)] = w_ref[0:HALF, :]
    wb[core, slot(1, x, y)] = w_ref[HALF:, :]

    def step_header(stab, norm):
        new = jnp.maximum(stab, top_loc[...])
        keep = jnp.exp(stab - new)
        add = jnp.exp(top_loc[...] - new)
        head_out[0:HEADS, :] = end_loc[...] + new
        head_out[HEADS:, :] = keep * norm + add * norm_loc[...]
        keep_scr[...] = jnp.concatenate([keep, keep], axis=1)
        add_scr[...] = jnp.concatenate([add, add], axis=1)

    @pl.when(me == 0)
    def _():
        head_in[...] = jnp.zeros((2 * HEADS, DK), F32)
        step_header(jnp.zeros((HEADS, DK), F32), jnp.zeros((HEADS, DK), F32))
        head_copy.start()
        for h in range(HEADS):

            def first(i, _, h=h):
                at = h * PIECES + i
                send[at] = (add_scr[h : h + 1, :] * part[at]).astype(BF16)
                piece_copy(at).start()
                return 0

            lax.fori_loop(0, PIECES, first, 0)

        gather_own()

        def clear(i, _):
            recv[i] = jnp.zeros((ROWS, DV), BF16)
            return 0

        lax.fori_loop(0, last, clear, 0)

    for h in range(HEADS):
        within_block(h, q_ref, k_ref, v_ref, run, gain, cm_scr, sv_scr, den_scr)
        gate_scr[:, h * DV : (h + 1) * DV] = jax.nn.sigmoid(
            og_ref[:, h * DV : (h + 1) * DV].astype(F32)
        )

    def consume(h):
        q = q_ref[:, h * DK : (h + 1) * DK]
        stab = head_in[h : h + 1, 0:T]
        norm = head_in[HEADS + h : HEADS + h + 1, :]
        top = jnp.maximum(stab, cm_scr[h])
        own = jnp.exp(cm_scr[h] - top)
        old = jnp.exp(stab - top)
        past = jnp.sum(q.astype(F32) * norm, axis=1, keepdims=True)
        den = own * den_scr[h] + old * past
        inv = 1.0 / jnp.maximum(jnp.abs(den), 1.0)
        own = own * inv
        old = old * inv
        state = recv[h * PIECES : (h + 1) * PIECES].reshape(DK, DV)
        carried = jnp.dot(q, state, preferred_element_type=F32)
        for c in range(DV // T):
            at = slice(c * T, (c + 1) * T)
            cell = own * sv_scr[h, :, at] + old * carried[:, at]
            hidden = cell.astype(BF16).astype(F32)
            cols = slice(h * DV + c * T, h * DV + (c + 1) * T)
            gated[:, at] = (hidden * gate_scr[:, cols]).astype(BF16)
        ks = slice(h * DV, (h + 1) * DV)

        def project(yy, _):
            rows = []
            for xx in range(NX):
                for cc in range(2):
                    rows.append(wa[cc, yy * NX + xx, :, ks])
                    rows.append(wb[cc, xx * NY + yy, :, ks])
            mine = lax.dot_general(
                gated[...],
                jnp.concatenate(rows, axis=0),
                (((1,), (1,)), ((), ())),
                preferred_element_type=F32,
            )
            if h > 0:
                mine = mine + acc[yy]
            if h < HEADS - 1:
                acc[yy] = mine
            else:
                at = pl.ds(pl.multiple_of(yy * 2 * NX * 2 * HALF, 2 * NX * 2 * HALF), 2 * NX * 2 * HALF)
                out_ref[:, at] = mine.astype(BF16)
            return 0

        lax.fori_loop(0, NY, project, 0)

    def chain():
        head_copy.wait_recv()
        step_header(head_in[0:HEADS, :], head_in[HEADS:, :])
        head_copy.start()
        for h in range(HEADS):

            def middle(i, _, h=h):
                at = h * PIECES + i
                piece_copy(at).wait_recv()
                new = keep_scr[h : h + 1, :] * recv[at].astype(F32) + add_scr[h : h + 1, :] * part[at]
                send[at] = new.astype(BF16)
                piece_copy(at).start()
                return 0

            lax.fori_loop(0, PIECES, middle, 0)

    ahead = jnp.int32(0)
    for first_plane in START:
        ahead = ahead + jnp.where(me >= first_plane, 1, 0)

    def phase(p, _):
        @pl.when(jnp.logical_and(p == ahead, jnp.logical_and(me > 0, me < size - 1)))
        def _():
            chain()

        for hops in range(1, 7):

            @pl.when(p == hops - 1)
            def _(hops=hops):
                gather_round(hops)

        return 0

    lax.fori_loop(0, 7, phase, 0)
    gather_end()

    @pl.when(me == size - 1)
    def _():
        head_copy.wait_recv()

    for h in range(HEADS):

        @pl.when(me == size - 1)
        def _(h=h):
            def final(i, _):
                piece_copy(h * PIECES + i).wait_recv()
                return 0

            lax.fori_loop(0, PIECES, final, 0)

        consume(h)

    @pl.when(me < size - 1)
    def _():
        head_copy.wait_send()

        pltpu.make_async_remote_copy(
            src_ref=send,
            dst_ref=recv,
            send_sem=send_sem.at[0],
            recv_sem=recv_sem.at[last],
            device_id={"sp": right},
            device_id_type=MESH,
        ).wait_send()


def cell(q, k, v, og, ig, fg, w):
    pieces = HEADS * PIECES
    return pl.pallas_call(
        cell_kernel,
        out_shape=jax.ShapeDtypeStruct((T, HEADS * DV), BF16),
        in_specs=[pl.BlockSpec(memory_space=pltpu.VMEM)] * 7,
        out_specs=pl.BlockSpec(memory_space=pltpu.VMEM),
        scratch_shapes=[
            pltpu.VMEM((pieces, ROWS, DV), F32),
            pltpu.VMEM((pieces, ROWS, DV), BF16),
            pltpu.VMEM((pieces, ROWS, DV), BF16),
            pltpu.VMEM((2 * HEADS, DK), F32),
            pltpu.VMEM((2 * HEADS, DK), F32),
            pltpu.VMEM((HEADS, DK), F32),
            pltpu.VMEM((HEADS, DK), F32),
            pltpu.VMEM((HEADS, DK), F32),
            pltpu.VMEM((HEADS, DV), F32),
            pltpu.VMEM((HEADS, DV), F32),
            pltpu.VMEM((HEADS, T, T), F32),
            pltpu.VMEM((HEADS, T, T), F32),
            pltpu.VMEM((HEADS, T, DV), F32),
            pltpu.VMEM((T, HEADS * DV), F32),
            pltpu.VMEM((T, DV), BF16),
            pltpu.VMEM((NY, T, 4 * NX * HALF), F32),
            pltpu.VMEM((2, NX * NY, HALF, HEADS * DV), BF16),
            pltpu.VMEM((2, NX * NY, HALF, HEADS * DV), BF16),
            pltpu.SemaphoreType.DMA((2,)),
            pltpu.SemaphoreType.DMA((pieces + 1,)),
            pltpu.SemaphoreType.DMA((NX * NY,)),
            pltpu.SemaphoreType.DMA((NX * NY,)),
            pltpu.SemaphoreType.DMA((2,)),
            pltpu.SemaphoreType.DMA((2,)),
            pltpu.SemaphoreType.DMA((2,)),
        ],
        compiler_params=pltpu.CompilerParams(collective_id=0, has_side_effects=True),
        cost_estimate=pl.CostEstimate(flops=10**11, bytes_accessed=2 * 10**7, transcendentals=0),
    )(q, k, v, og, ig, fg, w)


def body(queries, key_rows, values, out_gate, input_gate, forget_gate, out_weight):
    return cell(
        queries[0],
        key_rows[0],
        values[0],
        out_gate[0],
        input_gate[0],
        forget_gate[0],
        out_weight.T,
    )[None]


def solution(mesh):
    return jax.shard_map(
        body,
        mesh=mesh,
        in_specs=(
            P("dp", "sp", None),
            P("dp", "sp", None),
            P("dp", "sp", None),
            P("dp", "sp", None),
            P("dp", None, "sp"),
            P("dp", None, "sp"),
            P(None, "dp"),
        ),
        out_specs=P("dp", "sp", None),
        check_vma=False,
    )
```

```python
import functools

import jax
import jax.numpy as jnp
from jax import lax
from jax.experimental import pallas as pl
from jax.experimental.pallas import tpu as pltpu
from jax.sharding import PartitionSpec as P

MESH = pl.DeviceIdType.MESH
HEADS = 4
DK = 256
DV = 512
T = 128
ROWS = 16
PIECES = DK // ROWS
NX = 4
NY = 8
HALF = 16
ORDER = (
    (0, -1, 0), (0, 1, 0), (0, 0, -1), (0, 0, 1),
    (1, 0, 1), (1, 1, 0), (1, 0, -1), (1, -1, 0),
    (0, 2, 0), (0, -1, -1), (0, -1, 1), (1, -1, 1),
    (1, 1, 1), (0, 1, -1), (0, 1, 1), (1, -1, -1),
    (1, 2, 0), (0, 0, 2), (0, 0, -2), (1, 1, -1),
    (1, 0, 2), (1, 0, -2), (0, 2, -1), (0, 2, 1),
    (1, 2, 1), (1, 2, -1), (0, -1, 2), (0, -1, -2),
    (1, -1, 2), (1, 1, 2), (0, 1, 2), (0, 1, -2),
    (1, 1, -2), (1, -1, -2), (0, 0, -3), (0, 0, 3),
    (1, 0, -3), (1, 0, 3), (1, 2, 2), (0, 2, -2),
    (0, 2, 2), (1, 2, -2), (0, -1, -3), (0, -1, 3),
    (1, 1, -3), (1, -1, -3), (0, 1, -3), (0, 1, 3),
    (1, -1, 3), (1, 1, 3), (0, 0, 4), (0, 2, -3),
    (1, 0, 4), (0, -1, 4), (1, 2, -3), (0, 2, 3),
    (1, 2, 3), (0, 2, 4), (0, 1, 4), (1, 1, 4),
    (1, -1, 4), (1, 2, 4),
)
ACROSS = ((0, 1, 0), (1, 0, 3))
GROUP = 4
GROUPS = -(-len(ORDER) // GROUP)
SEGMENTS = 16
F32 = jnp.float32
BF16 = jnp.bfloat16


def local_terms(h, q_ref, k_ref, v_ref, run, gain, part, norm_loc, top_loc, cm_scr, kcol_scr):
    row = lax.broadcasted_iota(jnp.int32, (T, T), 0)
    col = lax.broadcasted_iota(jnp.int32, (T, T), 1)
    d = gain[h : h + 1, :] - run[h : h + 1, :]
    dd = jnp.broadcast_to(d, (T, T))
    running_top = jnp.max(jnp.where(col <= row, dd, -jnp.inf), axis=1, keepdims=True)
    d_col = jnp.sum(jnp.where(col == row, dd, 0.0), axis=1, keepdims=True)
    top = jnp.max(d, axis=1, keepdims=True)
    cm_scr[h] = jnp.broadcast_to(running_top, (T, T))
    top_loc[h : h + 1, :] = jnp.broadcast_to(top, (1, DK))
    keys = k_ref[:, h * DK : (h + 1) * DK].astype(F32) * (DK**-0.5)
    weighted = keys * jnp.exp(d_col - top)
    norm_loc[h : h + 1, :] = jnp.sum(weighted, axis=0, keepdims=True)
    state = lax.dot_general(
        weighted.astype(BF16),
        v_ref[:, h * DV : (h + 1) * DV],
        (((0,), (0,)), ((), ())),
        preferred_element_type=F32,
    )
    part[h * PIECES : (h + 1) * PIECES] = state.reshape(PIECES, ROWS, DV)


def within_block(h, q_ref, k_ref, v_ref, run, gain, cm_scr, sv_scr, den_scr):
    row = lax.broadcasted_iota(jnp.int32, (T, T), 0)
    col = lax.broadcasted_iota(jnp.int32, (T, T), 1)
    d = gain[h : h + 1, :] - run[h : h + 1, :]
    weight = jnp.where(col <= row, jnp.exp(jnp.minimum(d - cm_scr[h], 0.0)), 0.0)
    raw = lax.dot_general(
        q_ref[:, h * DK : (h + 1) * DK],
        k_ref[:, h * DK : (h + 1) * DK],
        (((1,), (1,)), ((), ())),
        preferred_element_type=F32,
    )
    scores = raw * (DK**-0.5) * weight
    den_scr[h] = jnp.broadcast_to(jnp.sum(scores, axis=1, keepdims=True), (T, T))
    high = scores.astype(BF16)
    low = (scores - high.astype(F32)).astype(BF16)
    values = v_ref[:, h * DV : (h + 1) * DV]
    sv_scr[h] = jnp.dot(high, values, preferred_element_type=F32) + jnp.dot(
        low, values, preferred_element_type=F32
    )


def cell_kernel(
    q_any,
    k_any,
    v_any,
    og_any,
    ig_any,
    fg_any,
    w_any,
    out_ref,
    q_ref,
    k_ref,
    v_ref,
    og_ref,
    ig_ref,
    fg_ref,
    w_ref,
    part,
    recv,
    send,
    head_in,
    head_out,
    norm_loc,
    top_loc,
    end_loc,
    keep_scr,
    add_scr,
    cm_scr,
    den_scr,
    sv_scr,
    gate_scr,
    gated,
    acc,
    wa,
    wb,
    send_sem,
    recv_sem,
    wa_recv,
    wb_recv,
    w_send,
    pair_send,
    pair_recv,
    load_sem,
):
    loads = {
        name: pltpu.make_async_copy(src, dst, load_sem.at[i])
        for i, (name, src, dst) in enumerate(
            (
                ("fg", fg_any, fg_ref),
                ("ig", ig_any, ig_ref),
                ("k", k_any, k_ref),
                ("v", v_any, v_ref),
                ("w", w_any, w_ref),
                ("q", q_any, q_ref),
                ("og", og_any, og_ref),
            )
        )
    }
    for load in loads.values():
        load.start()
    me = lax.axis_index("sp")
    size = lax.axis_size("sp")
    right = lax.rem(me + 1, size)
    left = lax.rem(me + size - 1, size)

    place = lax.axis_index("dp")
    core = lax.rem(place, 2)
    x = lax.rem(lax.div(place, 2), NX)
    y = lax.div(place, 2 * NX)

    def wrap(a, n):
        return lax.rem(a + n, n)

    def device(xx, yy, cc):
        return yy * (2 * NX) + xx * 2 + cc

    x_up = device(wrap(x + 1, NX), y, core)
    x_down = device(wrap(x - 1, NX), y, core)
    y_up = device(x, wrap(y + 1, NY), core)
    y_down = device(x, wrap(y - 1, NY), core)
    pair = device(x, y, 1 - core)

    barrier = pltpu.get_barrier_semaphore()

    @pl.when(me > 0)
    def _():
        pl.semaphore_signal(barrier, inc=1, device_id={"sp": left}, device_id_type=MESH)

    @pl.when(me < size - 1)
    def _():
        pl.semaphore_signal(barrier, inc=1, device_id={"sp": right}, device_id_type=MESH)

    for other in (x_up, x_down, y_up, y_down, pair):
        pl.semaphore_signal(barrier, inc=1, device_id={"dp": other}, device_id_type=MESH)

    kinds = ((wa, wa_recv, 0), (wb, wb_recv, 1))

    def slot(kind, xx, yy):
        return yy * NX + xx if kind == 0 else xx * NY + yy

    def block_send(kind, xx, yy, to, own=False):
        buf, arrived, which = kinds[kind]
        at = slot(kind, xx, yy)
        src = w_ref.at[pl.ds(kind * HALF, HALF)] if own else buf.at[core, at]
        pltpu.make_async_remote_copy(
            src_ref=src,
            dst_ref=buf.at[core, at],
            send_sem=w_send.at[which],
            recv_sem=arrived.at[at],
            device_id={"dp": to},
            device_id_type=MESH,
        ).start()

    def pair_copy(kind, xx, yy, own=False):
        buf, _, which = kinds[kind]
        at = slot(kind, xx, yy)
        src = w_ref.at[pl.ds(kind * HALF, HALF)] if own else buf.at[core, at]
        pltpu.make_async_remote_copy(
            src_ref=src,
            dst_ref=buf.at[core, at],
            send_sem=pair_send.at[which],
            recv_sem=pair_recv.at[which],
            device_id={"dp": pair},
            device_id_type=MESH,
        ).start()

    def block_wait(kind, xx, yy):
        buf, arrived, which = kinds[kind]
        at = slot(kind, xx, yy)
        pltpu.make_async_remote_copy(
            src_ref=buf.at[core, at],
            dst_ref=buf.at[core, at],
            send_sem=w_send.at[which],
            recv_sem=arrived.at[at],
            device_id={"dp": pair},
            device_id_type=MESH,
        ).wait_recv()

    turn = 1 - 2 * core

    def gather_own():
        for kind in range(2):
            for to in (x_up, x_down, y_up, y_down) if kind == 0 else (y_up, y_down, x_up, x_down):
                block_send(kind, x, y, to, own=True)
            pair_copy(kind, x, y, own=True)

    def first_event(o, t):
        xx, yy = wrap(x + o, NX), wrap(y - t, NY)
        block_wait(0, xx, yy)
        if t == 0 or t in (1, 2) or (t == 3 and o in (0, 1)):
            block_send(0, xx, yy, y_up)
        if t == 0 or t in (-1, -2) or (t == -3 and o in (-1, 2)):
            block_send(0, xx, yy, y_down)
        pair_copy(0, xx, yy)

    def second_event(o, t):
        xx, yy = wrap(x - o, NX), wrap(y - t, NY)
        block_wait(1, xx, yy)
        if o == 0 and t in (1, 2):
            block_send(1, xx, yy, y_up)
        if o == 0 and t in (-1, -2):
            block_send(1, xx, yy, y_down)
        if o == 0 or (o == 1 and t in (0, 1, 2, 3)):
            block_send(1, xx, yy, x_up)
        if o == 0 or (o == -1 and t not in (0, 1, 2, 3)):
            block_send(1, xx, yy, x_down)
        pair_copy(1, xx, yy)

    def gather_group(events):
        for kind, o, t in events:
            if kind == 0:
                first_event(o, t)
            else:
                second_event(o, t)
            if (kind, o, t) == ACROSS[0]:
                block_send(0, wrap(x - turn, NX), y, device(wrap(x + turn, NX), y, core))
            if (kind, o, t) == ACROSS[1]:
                block_send(1, x, wrap(y - 3 * turn, NY), device(x, wrap(y + turn, NY), core))

    def gather_end():
        for buf, _, which in kinds:
            whole = pltpu.make_async_remote_copy(
                src_ref=buf.at[core],
                dst_ref=buf.at[1 - core],
                send_sem=pair_send.at[which],
                recv_sem=pair_recv.at[which],
                device_id={"dp": pair},
                device_id_type=MESH,
            )
            whole.wait_recv()
            whole.wait_send()
            sent = buf.at[core, pl.ds(0, NX * NY - 1)]
            pltpu.make_async_remote_copy(
                src_ref=sent,
                dst_ref=sent,
                send_sem=w_send.at[which],
                recv_sem=pair_recv.at[which],
                device_id={"dp": pair},
                device_id_type=MESH,
            ).wait_send()

    def piece_copy(i):
        return pltpu.make_async_remote_copy(
            src_ref=send.at[i],
            dst_ref=recv.at[i],
            send_sem=send_sem.at[0],
            recv_sem=recv_sem.at[i],
            device_id={"sp": right},
            device_id_type=MESH,
        )

    last = HEADS * PIECES
    head_copy = pltpu.make_async_remote_copy(
        src_ref=head_out,
        dst_ref=head_in,
        send_sem=send_sem.at[1],
        recv_sem=recv_sem.at[last],
        device_id={"sp": right},
        device_id_type=MESH,
    )

    for name in ("fg", "ig", "k", "v"):
        loads[name].wait()
    gain = ig_ref[...].astype(F32)
    decay = -jnp.log1p(jnp.exp(-fg_ref[...].astype(F32)))
    row = lax.broadcasted_iota(jnp.int32, (T, T), 0)
    col = lax.broadcasted_iota(jnp.int32, (T, T), 1)
    upto = jnp.where(row <= col, 1.0, 0.0).astype(F32)
    run = jnp.dot(decay, upto, precision=lax.Precision.HIGHEST, preferred_element_type=F32)
    end_loc[...] = jnp.broadcast_to(run[:, T - 1 : T], (HEADS, DK))
    for h in range(HEADS):
        local_terms(h, q_ref, k_ref, v_ref, run, gain, part, norm_loc, top_loc, cm_scr, None)

    for name in ("w", "q", "og"):
        loads[name].wait()
    edge = jnp.logical_or(me == 0, me == size - 1)

    @pl.when(edge)
    def _():
        pl.semaphore_wait(barrier, 6)

    @pl.when(jnp.logical_not(edge))
    def _():
        pl.semaphore_wait(barrier, 7)
    @pl.when(me > 0)
    def _():
        gather_own()

    wa[core, slot(0, x, y)] = w_ref[0:HALF, :]
    wb[core, slot(1, x, y)] = w_ref[HALF:, :]

    def step_header(stab, norm):
        new = jnp.maximum(stab, top_loc[...])
        keep = jnp.exp(stab - new)
        add = jnp.exp(top_loc[...] - new)
        head_out[0:HEADS, :] = end_loc[...] + new
        head_out[HEADS:, :] = keep * norm + add * norm_loc[...]
        keep_scr[...] = jnp.concatenate([keep, keep], axis=1)
        add_scr[...] = jnp.concatenate([add, add], axis=1)

    @pl.when(me == 0)
    def _():
        head_in[...] = jnp.zeros((2 * HEADS, DK), F32)
        step_header(jnp.zeros((HEADS, DK), F32), jnp.zeros((HEADS, DK), F32))
        head_copy.start()
        for h in range(HEADS):

            def first(i, _, h=h):
                at = h * PIECES + i
                send[at] = (add_scr[h : h + 1, :] * part[at]).astype(BF16)
                piece_copy(at).start()
                return 0

            lax.fori_loop(0, PIECES, first, 0)

        gather_own()

        def clear(i, _):
            recv[i] = jnp.zeros((ROWS, DV), BF16)
            return 0

        lax.fori_loop(0, last, clear, 0)

    for h in range(HEADS):
        within_block(h, q_ref, k_ref, v_ref, run, gain, cm_scr, sv_scr, den_scr)
        gate_scr[:, h * DV : (h + 1) * DV] = jax.nn.sigmoid(
            og_ref[:, h * DV : (h + 1) * DV].astype(F32)
        )

    def consume(h):
        q = q_ref[:, h * DK : (h + 1) * DK]
        stab = head_in[h : h + 1, 0:T]
        norm = head_in[HEADS + h : HEADS + h + 1, :]
        top = jnp.maximum(stab, cm_scr[h])
        own = jnp.exp(cm_scr[h] - top)
        old = jnp.exp(stab - top)
        past = jnp.sum(q.astype(F32) * norm, axis=1, keepdims=True)
        den = own * den_scr[h] + old * past
        inv = 1.0 / jnp.maximum(jnp.abs(den), 1.0)
        own = own * inv
        old = old * inv
        state = recv[h * PIECES : (h + 1) * PIECES].reshape(DK, DV)
        carried = jnp.dot(q, state, preferred_element_type=F32)
        for c in range(DV // T):
            at = slice(c * T, (c + 1) * T)
            cell = own * sv_scr[h, :, at] + old * carried[:, at]
            hidden = cell.astype(BF16).astype(F32)
            cols = slice(h * DV + c * T, h * DV + (c + 1) * T)
            gated[:, at] = (hidden * gate_scr[:, cols]).astype(BF16)
        ks = slice(h * DV, (h + 1) * DV)

        def project(yy, _):
            rows = []
            for xx in range(NX):
                for cc in range(2):
                    rows.append(wa[cc, yy * NX + xx, :, ks])
                    rows.append(wb[cc, xx * NY + yy, :, ks])
            mine = lax.dot_general(
                jnp.concatenate(rows, axis=0),
                gated[...],
                (((1,), (1,)), ((), ())),
                preferred_element_type=F32,
            )
            if h > 0:
                mine = mine + acc[yy]
            if h < HEADS - 1:
                acc[yy] = mine
            else:
                at = pl.ds(pl.multiple_of(yy * 2 * NX * 2 * HALF, 2 * NX * 2 * HALF), 2 * NX * 2 * HALF)
                out_ref[:, at] = jnp.transpose(mine).astype(BF16)
            return 0

        lax.fori_loop(0, NY, project, 0)

    def chain(segment):
        @pl.when(segment == 0)
        def _():
            head_copy.wait_recv()
            step_header(head_in[0:HEADS, :], head_in[HEADS:, :])
            head_copy.start()

        h = lax.div(segment * HEADS, SEGMENTS)
        keep = keep_scr[pl.ds(h, 1), :]
        add = add_scr[pl.ds(h, 1), :]

        def middle(i, _):
            at = segment * (last // SEGMENTS) + i
            piece_copy(at).wait_recv()
            send[at] = (keep * recv[at].astype(F32) + add * part[at]).astype(BF16)
            piece_copy(at).start()
            return 0

        lax.fori_loop(0, last // SEGMENTS, middle, 0)

    inner = jnp.logical_and(me > 0, me < size - 1)
    begin = lax.div(4 * me + 2, 5)

    def phase(p, done):
        segment = p - begin
        busy = jnp.logical_and(inner, jnp.logical_and(segment >= 0, segment < SEGMENTS))

        @pl.when(busy)
        def _():
            chain(segment)

        free = jnp.logical_or(jnp.logical_not(busy), lax.rem(p - begin + 64, 2) == 1)
        for g in range(GROUPS):

            @pl.when(jnp.logical_and(free, done == g))
            def _(g=g):
                gather_group(ORDER[g * GROUP : (g + 1) * GROUP])

        return done + jnp.where(free, 1, 0)

    lax.fori_loop(0, GROUPS + SEGMENTS // 2 + 4, phase, jnp.int32(0))
    gather_end()

    @pl.when(me == size - 1)
    def _():
        head_copy.wait_recv()

    for h in range(HEADS):

        @pl.when(me == size - 1)
        def _(h=h):
            def final(i, _):
                piece_copy(h * PIECES + i).wait_recv()
                return 0

            lax.fori_loop(0, PIECES, final, 0)

        consume(h)

    @pl.when(me < size - 1)
    def _():
        head_copy.wait_send()

        pltpu.make_async_remote_copy(
            src_ref=send,
            dst_ref=recv,
            send_sem=send_sem.at[0],
            recv_sem=recv_sem.at[last],
            device_id={"sp": right},
            device_id_type=MESH,
        ).wait_send()


def cell(q, k, v, og, ig, fg, w):
    pieces = HEADS * PIECES
    return pl.pallas_call(
        cell_kernel,
        out_shape=jax.ShapeDtypeStruct((T, HEADS * DV), BF16),
        in_specs=[pl.BlockSpec(memory_space=pltpu.HBM)] * 7,
        out_specs=pl.BlockSpec(memory_space=pltpu.VMEM),
        scratch_shapes=[pltpu.VMEM(a.shape, a.dtype) for a in (q, k, v, og, ig, fg, w)]
        + [
            pltpu.VMEM((pieces, ROWS, DV), F32),
            pltpu.VMEM((pieces, ROWS, DV), BF16),
            pltpu.VMEM((pieces, ROWS, DV), BF16),
            pltpu.VMEM((2 * HEADS, DK), F32),
            pltpu.VMEM((2 * HEADS, DK), F32),
            pltpu.VMEM((HEADS, DK), F32),
            pltpu.VMEM((HEADS, DK), F32),
            pltpu.VMEM((HEADS, DK), F32),
            pltpu.VMEM((HEADS, DV), F32),
            pltpu.VMEM((HEADS, DV), F32),
            pltpu.VMEM((HEADS, T, T), F32),
            pltpu.VMEM((HEADS, T, T), F32),
            pltpu.VMEM((HEADS, T, DV), F32),
            pltpu.VMEM((T, HEADS * DV), F32),
            pltpu.VMEM((T, DV), BF16),
            pltpu.VMEM((NY, 4 * NX * HALF, T), F32),
            pltpu.VMEM((2, NX * NY, HALF, HEADS * DV), BF16),
            pltpu.VMEM((2, NX * NY, HALF, HEADS * DV), BF16),
            pltpu.SemaphoreType.DMA((2,)),
            pltpu.SemaphoreType.DMA((pieces + 1,)),
            pltpu.SemaphoreType.DMA((NX * NY,)),
            pltpu.SemaphoreType.DMA((NX * NY,)),
            pltpu.SemaphoreType.DMA((2,)),
            pltpu.SemaphoreType.DMA((2,)),
            pltpu.SemaphoreType.DMA((2,)),
            pltpu.SemaphoreType.DMA((7,)),
        ],
        compiler_params=pltpu.CompilerParams(collective_id=0, has_side_effects=True),
        cost_estimate=pl.CostEstimate(flops=10**11, bytes_accessed=2 * 10**7, transcendentals=0),
    )(q, k, v, og, ig, fg, w)


def body(queries, key_rows, values, out_gate, input_gate, forget_gate, out_weight):
    return cell(
        queries[0],
        key_rows[0],
        values[0],
        out_gate[0],
        input_gate[0],
        forget_gate[0],
        out_weight.T,
    )[None]


def solution(mesh):
    return jax.shard_map(
        body,
        mesh=mesh,
        in_specs=(
            P("dp", "sp", None),
            P("dp", "sp", None),
            P("dp", "sp", None),
            P("dp", "sp", None),
            P("dp", None, "sp"),
            P("dp", None, "sp"),
            P(None, "dp"),
        ),
        out_specs=P("dp", "sp", None),
        check_vma=False,
    )
```
